128 devices in a mesh: sp: 32 (over z, y, core), tp: 4 (over x).
Axes of the slice: x: 4, y: 4, z: 4, core: 2. Of those that a mesh axis runs over, the one named last changes fastest.
Arguments:
- residual: bfloat16 [32768, 2048], P('sp'), may hold values from -6 to 6
- small_heads: bfloat16 [32768, 1024], P('sp', 'tp'), may hold values from -6 to 6
- large_heads: bfloat16 [32768, 1024], P('sp', 'tp'), may hold values from -6 to 6
- state_keys: bfloat16 [32768, 8, 128], P('sp', 'tp'), may hold values from -6 to 6
- state_queries: bfloat16 [32768, 8, 128], P('sp', 'tp'), may hold values from -6 to 6
- small_gate: bfloat16 [32768, 1024], P('sp', 'tp'), may hold values from -6 to 6
- large_gate: bfloat16 [32768, 1024], P('sp', 'tp'), may hold values from -6 to 6
- small_step: float32 [32768, 16], P('sp', 'tp'), may hold values from -3 to 2
- large_step: float32 [32768, 8], P('sp', 'tp'), may hold values from -3 to 2
- small_taps: bfloat16 [4, 1024], P(None, 'tp'), may hold values from -3 to 3
- large_taps: bfloat16 [4, 1024], P(None, 'tp'), may hold values from -3 to 3
- key_taps: bfloat16 [4, 8, 128], P(None, 'tp'), may hold values from -3 to 3
- query_taps: bfloat16 [4, 8, 128], P(None, 'tp'), may hold values from -3 to 3
- small_decay: float32 [16], P('tp'), may hold values from -12 to -2, as said below
- large_decay: float32 [8], P('tp'), may hold values from -12 to -2, as said below
- small_gain: bfloat16 [1024], P('tp'), may hold values from 0.099609375 to 1.8984375
- large_gain: bfloat16 [1024], P('tp'), may hold values from 0.099609375 to 1.8984375
- small_out: bfloat16 [1024, 2048], P('tp'), may hold values from -0.125 to 0.125
- large_out: bfloat16 [1024, 2048], P('tp'), may hold values from -0.125 to 0.125
- mixer_gain: bfloat16 [2048], replicated, may hold values from 0.099609375 to 1.8984375
- ffn_in_gain: bfloat16 [2048], replicated, may hold values from 0.099609375 to 1.8984375
- gate_proj: bfloat16 [2048, 5632], P('sp', 'tp'), may hold values from -0.125 to 0.125
- up_proj: bfloat16 [2048, 5632], P('sp', 'tp'), may hold values from -0.125 to 0.125
- down_proj: bfloat16 [2048, 5632], P('sp', 'tp'), may hold values from -0.078125 to 0.078125
- ffn_out_gain: bfloat16 [2048], replicated, may hold values from 0.099609375 to 1.8984375
Outputs:
- updated: bfloat16 [32768, 2048], P(('sp', 'tp'))
The draws below stay inside these ranges and needn't reach their ends.
Inputs may be any that keep to these rules, and one draw needn't show every extreme that they name: `small_decay`: log decay rates of the first group. `large_decay`: log decay rates of the second group.
All inputs are finite; a program needn't handle non-finite values.
Results may differ from the reference program's by a relative error of at most 0.014.
Values may be sent and summed in bfloat16 or wider, within the bound.
No kernel may reach another device: no remote copies, remote signals or barrier semaphores. Data moves between devices by JAX's collectives and lax.ppermute only.
A program may use at most 192 MiB of HBM per device.

```python
import jax
import jax.numpy as jnp
from jax import lax

D = 2048
FF = 5632
HA = 16
PA = 64
HB = 8
PB = 128
GROUPS = 8
STATE = 128
CONV = 4
BLOCK = 128
TOK_DEV = 1024
TOKENS = 32768
HEAD_BLOCKS = 4


def step_law(key, heads, salt):
    rows = jnp.arange(TOKENS, dtype=jnp.int32) // TOK_DEV
    offset_key = jax.random.fold_in(key, 101)
    jitter_key = jax.random.fold_in(key, salt)
    offsets = jax.random.uniform(offset_key, (TOKENS // TOK_DEV,), jnp.float32, -1.5, 0.5)
    jitter = jnp.clip(0.5 * jax.random.normal(jitter_key, (TOKENS, heads), jnp.float32), -1.5, 1.5)
    return offsets[rows][:, None] + jitter


def decay_law(key, heads, salt):
    base_key = jax.random.fold_in(key, salt)
    order_key, slow_key, fast_key = jax.random.split(base_key, 3)
    fast_count = heads // 2
    ranks = jax.random.permutation(order_key, heads)
    slow_values = jnp.log(jax.random.uniform(slow_key, (heads,), jnp.float32, 0.25, 1.5) / TOKENS)
    fast_values = jnp.log(jax.random.uniform(fast_key, (heads,), jnp.float32, 1.0 / 60.0, 1.0 / 20.0))
    return jnp.where(ranks < fast_count, fast_values, slow_values)


def draw_small_step(key, part):
    return step_law(key, HA, 11)


def draw_large_step(key, part):
    return step_law(key, HB, 12)


def draw_small_decay(key, part):
    return decay_law(key, HA, 21)


def draw_large_decay(key, part):
    return decay_law(key, HB, 22)


def shard_levels(rng, shape, pieces, low, top_value):
    def one(position, parts):
        draws = jax.random.uniform(jax.random.fold_in(jax.random.fold_in(rng, 6), position), (parts,), jnp.float32, low / len(pieces), top_value / len(pieces))
        return jnp.repeat(jnp.exp(draws), shape[position] // parts).reshape((-1,) + (1,) * (len(shape) - position - 1))

    loudness = one(*pieces[0])
    for cut in pieces[1:]:
        loudness = loudness * one(*cut)
    return loudness


def scatter_about(rng, shape, width, bound, cuts=(), kind=jnp.bfloat16):
    level = shard_levels(rng, shape, cuts, -0.22, 0.18) if cuts else 1.0
    drawn = jax.random.normal(rng, shape, jnp.float32) * width * level
    return jnp.minimum(jnp.maximum(drawn, -bound), bound).astype(kind)


def setup_inputs(seed: int = 0) -> dict:
    arg_keys = jax.random.split(jax.random.key(seed), 26)
    return {
        "residual": scatter_about(arg_keys[0], (TOKENS, D), 1.0, 6.0, ((0, 32),)),
        "small_heads": scatter_about(arg_keys[1], (TOKENS, HA * PA), 1.0, 6.0, ((0, 32), (1, 4))),
        "large_heads": scatter_about(arg_keys[2], (TOKENS, HB * PB), 1.0, 6.0, ((0, 32), (1, 4))),
        "state_keys": scatter_about(arg_keys[3], (TOKENS, GROUPS, STATE), 1.0, 6.0, ((0, 32), (1, 4))),
        "state_queries": scatter_about(arg_keys[4], (TOKENS, GROUPS, STATE), 1.0, 6.0, ((0, 32), (1, 4))),
        "small_gate": scatter_about(arg_keys[5], (TOKENS, HA * PA), 1.0, 6.0, ((0, 32), (1, 4))),
        "large_gate": scatter_about(arg_keys[6], (TOKENS, HB * PB), 1.0, 6.0, ((0, 32), (1, 4))),
        "small_step": draw_small_step(jax.random.fold_in(arg_keys[25], 71), 0),
        "large_step": draw_large_step(jax.random.fold_in(arg_keys[25], 71), 0),
        "small_taps": scatter_about(arg_keys[9], (CONV, HA * PA), CONV ** -0.5, 3.0, ((1, 4),)),
        "large_taps": scatter_about(arg_keys[10], (CONV, HB * PB), CONV ** -0.5, 3.0, ((1, 4),)),
        "key_taps": scatter_about(arg_keys[11], (CONV, GROUPS, STATE), CONV ** -0.5, 3.0, ((1, 4),)),
        "query_taps": scatter_about(arg_keys[12], (CONV, GROUPS, STATE), CONV ** -0.5, 3.0, ((1, 4),)),
        "small_decay": draw_small_decay(jax.random.fold_in(arg_keys[25], 71), 0),
        "large_decay": draw_large_decay(jax.random.fold_in(arg_keys[25], 71), 0),
        "small_gain": jnp.clip(1.0 + 0.18 * jax.random.normal(arg_keys[15], (HA * PA,), jnp.float32), 0.099609375, 1.8984375).astype(jnp.bfloat16),
        "large_gain": jnp.clip(1.0 + 0.18 * jax.random.normal(arg_keys[16], (HB * PB,), jnp.float32), 0.099609375, 1.8984375).astype(jnp.bfloat16),
        "small_out": scatter_about(arg_keys[17], (HA * PA, D), (HA * PA + HB * PB) ** -0.5, 0.125, ((0, 4),)),
        "large_out": scatter_about(arg_keys[18], (HB * PB, D), (HA * PA + HB * PB) ** -0.5, 0.125, ((0, 4),)),
        "mixer_gain": jnp.clip(1.0 + 0.18 * jax.random.normal(arg_keys[19], (D,), jnp.float32), 0.099609375, 1.8984375).astype(jnp.bfloat16),
        "ffn_in_gain": jnp.clip(1.0 + 0.18 * jax.random.normal(arg_keys[20], (D,), jnp.float32), 0.099609375, 1.8984375).astype(jnp.bfloat16),
        "gate_proj": scatter_about(arg_keys[21], (D, FF), D ** -0.5, 0.125, ((0, 32), (1, 4))),
        "up_proj": scatter_about(arg_keys[22], (D, FF), D ** -0.5, 0.125, ((0, 32), (1, 4))),
        "down_proj": scatter_about(arg_keys[23], (D, FF), FF ** -0.5, 0.078125, ((0, 32), (1, 4))),
        "ffn_out_gain": jnp.clip(1.0 + 0.18 * jax.random.normal(arg_keys[24], (D,), jnp.float32), 0.099609375, 1.8984375).astype(jnp.bfloat16),
    }


EPS = 1e-06

def rounded(values):
    return lax.optimization_barrier(values.astype(jnp.bfloat16)).astype(jnp.float32)

def causal_taps(extended, tap_weights, length):
    kernel_len = tap_weights.shape[0]
    summed = jnp.zeros((length,) + extended.shape[1:], jnp.float32)
    for offset in range(kernel_len):
        window_rows = extended[offset:offset + length].astype(jnp.float32)
        summed = summed + tap_weights[offset].astype(jnp.float32) * window_rows
    return jax.nn.silu(summed).astype(jnp.bfloat16)

def block_pass(values, key_rows, queries, step_sizes, decay_rates):
    length, groups, head_count, head_dim = values.shape
    block_count = length // BLOCK
    state_len = key_rows.shape[-1]
    log_decay = -step_sizes * decay_rates
    causal = jnp.tril(jnp.ones((BLOCK, BLOCK), dtype=bool))
    highest = lax.Precision.HIGHEST

    def one_block(carry_state, block):
        block_values, block_keys, block_queries, block_steps, block_decay = block
        values_wide = block_values.astype(jnp.float32)
        keys_wide = block_keys.astype(jnp.float32)
        queries_wide = block_queries.astype(jnp.float32)
        cumulative = jnp.cumsum(block_decay, axis=0)
        scores = jnp.einsum('lgn,sgn->gls', queries_wide, keys_wide, precision=highest)
        cum_heads = jnp.transpose(cumulative, (1, 2, 0))
        gap_matrix = cum_heads[:, :, :, None] - cum_heads[:, :, None, :]
        decays = jnp.exp(jnp.where(causal, gap_matrix, -jnp.inf))
        step_heads = jnp.transpose(block_steps, (1, 2, 0))[:, :, None, :]
        weights = rounded(scores[:, None] * decays * step_heads)
        inside = jnp.einsum('ghls,sghp->lghp', weights, values_wide, precision=highest)
        carried = jnp.einsum('lgn,ghpn->lghp', queries_wide, carry_state, precision=highest)
        carried = carried * jnp.exp(cumulative)[..., None]
        tail_sum = cumulative[-1]
        scaled = rounded(values_wide * (block_steps * jnp.exp(tail_sum - cumulative))[..., None])
        fresh_state = jnp.einsum('lghp,lgn->ghpn', scaled, keys_wide, precision=highest)
        next_state = carry_state * jnp.exp(tail_sum)[..., None, None] + fresh_state
        return (next_state, inside + carried)
    blocked = (values.reshape(block_count, BLOCK, groups, head_count, head_dim), key_rows.reshape(block_count, BLOCK, groups, state_len), queries.reshape(block_count, BLOCK, groups, state_len), step_sizes.reshape(block_count, BLOCK, groups, head_count), log_decay.reshape(block_count, BLOCK, groups, head_count))
    start_state = jnp.zeros((groups, head_count, head_dim, state_len), jnp.float32)
    end_state, outputs = lax.scan(one_block, start_state, blocked)
    return outputs.reshape(length, groups, head_count, head_dim)

def head_group(values, key_rows, queries, step_raw, decay_log):
    length = values.shape[0]
    head_count = step_raw.shape[1]
    groups = key_rows.shape[1]
    per_group = head_count // groups
    head_dim = values.shape[1] // head_count
    step_sizes = jax.nn.softplus(step_raw.astype(jnp.float32)).reshape(length, groups, per_group)
    decay_rates = jnp.exp(decay_log.astype(jnp.float32)).reshape(groups, per_group)
    return block_pass(values.reshape(length, groups, per_group, head_dim), key_rows, queries, step_sizes, decay_rates)

def unit_rms(values):
    return values * lax.rsqrt(lax.optimization_barrier(jnp.mean(values * values, axis=-1, keepdims=True)) + EPS)

def gate_and_norm(mixed_heads, gate_raw, gain):
    length, groups, per_group, head_dim = mixed_heads.shape
    gated = mixed_heads.reshape(length, -1) * jax.nn.silu(gate_raw.astype(jnp.float32))
    normed = unit_rms(gated.reshape(length, groups * per_group, head_dim))
    return (normed.reshape(length, -1) * gain.astype(jnp.float32)).astype(jnp.bfloat16)

def blockwise_sum(pairs, length, features):
    summed = jnp.zeros((length, features), jnp.float32)
    for index in range(HEAD_BLOCKS):
        partial_value = jnp.zeros((length, features), jnp.float32)
        for left, right in pairs:
            cols = left.shape[1] // HEAD_BLOCKS
            partial_value = partial_value + jnp.dot(left[:, index * cols:(index + 1) * cols], right[index * cols:(index + 1) * cols], preferred_element_type=jnp.float32)
        summed = summed + rounded(partial_value)
    return summed

def reference(residual, small_heads, large_heads, state_keys, state_queries, small_gate, large_gate, small_step, large_step, small_taps, large_taps, key_taps, query_taps, small_decay, large_decay, small_gain, large_gain, small_out, large_out, mixer_gain, ffn_in_gain, gate_proj, up_proj, down_proj, ffn_out_gain):
    length = residual.shape[0]
    halo_rows = small_taps.shape[0] - 1

    def extended(values):
        return jnp.concatenate([jnp.zeros((halo_rows,) + values.shape[1:], values.dtype), values], axis=0)
    small_conv = causal_taps(extended(small_heads), small_taps, length)
    large_conv = causal_taps(extended(large_heads), large_taps, length)
    key_conv = causal_taps(extended(state_keys), key_taps, length)
    query_conv = causal_taps(extended(state_queries), query_taps, length)
    small_mix = head_group(small_conv, key_conv[:, 0::2], query_conv[:, 0::2], small_step, small_decay)
    large_mix = head_group(large_conv, key_conv[:, 1::2], query_conv[:, 1::2], large_step, large_decay)
    small_normed = gate_and_norm(small_mix, small_gate, small_gain)
    large_normed = gate_and_norm(large_mix, large_gate, large_gain)
    mix = blockwise_sum([(small_normed, small_out), (large_normed, large_out)], length, D)
    mixed = residual.astype(jnp.float32) + unit_rms(mix) * mixer_gain.astype(jnp.float32)
    normed_in = (unit_rms(mixed) * ffn_in_gain.astype(jnp.float32)).astype(jnp.bfloat16)
    gate = jnp.dot(normed_in, gate_proj, preferred_element_type=jnp.float32)
    up_values = jnp.dot(normed_in, up_proj, preferred_element_type=jnp.float32)
    hidden = (jax.nn.silu(gate) * up_values).astype(jnp.bfloat16)
    ffn = blockwise_sum([(hidden, jnp.transpose(down_proj))], length, D)
    updated = mixed + 0.5 * unit_rms(ffn) * ffn_out_gain.astype(jnp.float32)
    return updated.astype(jnp.bfloat16)
```

```python
import jax
import jax.numpy as jnp
from jax import lax
from jax.experimental import pallas as pl
from jax.experimental.pallas import tpu as pltpu
from jax.sharding import Mesh
from jax.sharding import PartitionSpec as P

BLOCK = 128
HALO = 16
EPS = 1e-06
F32 = jnp.float32
BF16 = jnp.bfloat16


def cost(us):
    return pl.CostEstimate(flops=int(us * 2.5e8), bytes_accessed=int(us * 1e5), transcendentals=0)


def column_pairs(wide):
    lane = lax.broadcasted_iota(jnp.int32, wide[0].shape, 1)
    low = lane < 64
    return jnp.concatenate(
        [jnp.where(low, wide[0], wide[1]), jnp.where(low, wide[2], wide[3]), wide[4], wide[5]],
        axis=1,
    )


def pack_body(small, large, keys, queries, out, wide):
    out[:, 0:256] = small[...]
    out[:, 256:512] = large[...]
    for n, ref in enumerate((keys, queries)):
        wide[...] = ref[...].astype(F32)
        for g in range(2):
            at = 512 + 256 * n + 128 * g
            out[:, at : at + 128] = wide[pl.ds(g, HALO, stride=2), :].astype(BF16)


def pack_halo(small, large, keys, queries):
    last = small.shape[0] // HALO - 1
    return pl.pallas_call(
        pack_body,
        grid=(1,),
        in_specs=[
            pl.BlockSpec((HALO, 256), lambda i: (last, 0)),
            pl.BlockSpec((HALO, 256), lambda i: (last, 0)),
            pl.BlockSpec((2 * HALO, 128), lambda i: (last, 0)),
            pl.BlockSpec((2 * HALO, 128), lambda i: (last, 0)),
        ],
        out_specs=pl.BlockSpec((HALO, 1024), lambda i: (0, 0)),
        out_shape=jax.ShapeDtypeStruct((HALO, 1024), BF16),
        scratch_shapes=[pltpu.VMEM((2 * HALO, 128), F32)],
        name="pack_halo",
        cost_estimate=cost(1),
    )(small, large, keys, queries)


def put_state(ref, state, total):
    ref[0:BLOCK, :] = state.astype(BF16)
    high = total.astype(BF16)
    low = (total - high.astype(F32)).astype(BF16)
    ref[BLOCK : BLOCK + 16, :] = jnp.concatenate([high, low], axis=0)


def get_state(piece):
    piece = piece.astype(F32)
    return piece[0:BLOCK, :], piece[BLOCK : BLOCK + 8, :] + piece[BLOCK + 8 : BLOCK + 16, :]


def then(earlier, later):
    return earlier[0] * jnp.exp(later[1][0:1, :]) + later[0], earlier[1] + later[1]


def mixer_body(
    core,
    small_decay,
    large_decay,
    halo,
    small,
    large,
    keys,
    queries,
    small_step,
    large_step,
    small_taps,
    large_taps,
    key_taps,
    query_taps,
    mix_out,
    query_out,
    cum_out,
    keep_out,
    send_out,
    ext,
    wide,
    rows,
    state,
    total_rows,
    total_cols,
):
    step = pl.program_id(0)

    @pl.when(step == 0)
    def _():
        ext[0:8, :] = halo[...].astype(F32)[HALO - 8 :, :]
        state[...] = jnp.zeros_like(state)
        total_rows[...] = jnp.zeros_like(total_rows)
        total_cols[...] = jnp.zeros_like(total_cols)

    @pl.when(step > 0)
    def _():
        ext[0:8, :] = ext[BLOCK : BLOCK + 8, :]

    ext[8:, 0:256] = small[...].astype(F32)
    ext[8:, 256:512] = large[...].astype(F32)
    for n, ref in enumerate((keys, queries)):
        wide[n] = ref[...].astype(F32)
        for g in range(2):
            at = 512 + 256 * n + 128 * g
            ext[8:, at : at + 128] = wide[n, pl.ds(g, BLOCK, stride=2), :]

    kt = key_taps[...].astype(F32)
    qt = query_taps[...].astype(F32)
    st = small_taps[...].astype(F32)
    lt = large_taps[...].astype(F32)

    def conv(at, tap_rows):
        summed = tap_rows[0] * ext[5 : 5 + BLOCK, at : at + 128]
        for k in range(1, 4):
            summed = summed + tap_rows[k] * ext[5 + k : 5 + k + BLOCK, at : at + 128]
        return (summed * jax.nn.sigmoid(summed)).astype(BF16)

    values = [conv(128 * n, [st[k : k + 1, 128 * n : 128 * n + 128] for k in range(4)]) for n in range(2)]
    values += [
        conv(256 + 128 * n, [lt[k : k + 1, 128 * n : 128 * n + 128] for k in range(4)]) for n in range(2)
    ]
    key = [conv(512 + 128 * g, [kt[2 * k + g : 2 * k + g + 1, :] for k in range(4)]) for g in range(2)]
    query = [conv(768 + 128 * g, [qt[2 * k + g : 2 * k + g + 1, :] for k in range(4)]) for g in range(2)]
    query_out[...] = jnp.concatenate(query, axis=1)

    rows[0, 0:4, :] = small_step[...]
    rows[0, 4:6, :] = large_step[...]
    rows[0, 6:8, :] = jnp.zeros((2, BLOCK), F32)
    raw = rows[0]
    dt = jnp.maximum(raw, 0.0) + jnp.log1p(jnp.exp(-jnp.abs(raw)))
    for h in range(8):
        if h < 6:
            log_rate = small_decay[h] if h < 4 else large_decay[h - 4]
            rows[1, h : h + 1, :] = jnp.exp(jnp.full((1, BLOCK), log_rate, F32))
        else:
            rows[1, h : h + 1, :] = jnp.zeros((1, BLOCK), F32)
    decay = -dt * rows[1]
    r = lax.broadcasted_iota(jnp.int32, (BLOCK, BLOCK), 0)
    c = lax.broadcasted_iota(jnp.int32, (BLOCK, BLOCK), 1)
    upper = (r <= c).astype(F32)
    causal = c <= r
    cum = jnp.dot(decay, upper, precision=lax.Precision.HIGHEST, preferred_element_type=F32)
    tail = jnp.broadcast_to(cum[:, BLOCK - 1 : BLOCK], cum.shape)
    cum_out[...] = cum + total_rows[...]
    total_rows[...] = total_rows[...] + tail
    factor = dt * jnp.exp(tail - cum)
    cum_t = cum.T
    factor_t = factor.T
    cum_b = [jnp.broadcast_to(cum_t[:, h : h + 1], (BLOCK, BLOCK)) for h in range(6)]
    factor_b = [jnp.broadcast_to(factor_t[:, h : h + 1], (BLOCK, BLOCK)) for h in range(6)]
    cum_cols = column_pairs(cum_b)
    factor_cols = column_pairs(factor_b)
    tail_cols = cum_cols[BLOCK - 1 : BLOCK, :]

    scores = [
        lax.dot_general(query[g], key[g], (((1,), (1,)), ((), ())), preferred_element_type=F32)
        for g in range(2)
    ]
    inside = []
    for h in range(6):
        gap = cum_b[h] - cum[h : h + 1, :]
        decays = jnp.exp(jnp.where(causal, gap, -jnp.inf))
        weights = (scores[h // 4] * decays * dt[h : h + 1, :]).astype(BF16)
        if h < 4:
            inside.append(
                jnp.dot(weights, values[h // 2], preferred_element_type=F32)
            )
        else:
            inside.append(jnp.dot(weights, values[h - 2], preferred_element_type=F32))
    inside = column_pairs(inside)
    before = state[...].astype(BF16)
    carried = jnp.concatenate(
        [jnp.dot(query[g], before[:, 256 * g : 256 * g + 256], preferred_element_type=F32) for g in range(2)],
        axis=1,
    )
    mix_out[...] = inside + carried * jnp.exp(cum_cols)
    scaled = (jnp.concatenate(values, axis=1).astype(F32) * factor_cols).astype(BF16)
    fresh = jnp.concatenate(
        [
            lax.dot_general(
                key[g], scaled[:, 256 * g : 256 * g + 256], (((0,), (0,)), ((), ())), preferred_element_type=F32
            )
            for g in range(2)
        ],
        axis=1,
    )
    state[...] = state[...] * jnp.exp(tail_cols) + fresh
    total_cols[...] = total_cols[...] + tail_cols

    @pl.when(step == pl.num_programs(0) - 1)
    def _():
        first = core[0] == 0
        for ref, own in ((keep_out, first), (send_out, jnp.logical_not(first))):
            put_state(
                ref,
                jnp.where(own, state[:, 0:256], state[:, 256:512]),
                jnp.where(own, total_cols[:, 0:256], total_cols[:, 256:512]),
            )


def mixer(core, halo, small, large, keys, queries, small_step, large_step, small_taps, large_taps, key_taps, query_taps, small_decay, large_decay):
    length = small.shape[0]
    blocks = length // BLOCK
    whole = lambda *shape: pl.BlockSpec(shape, lambda i: (0,) * len(shape))
    return pl.pallas_call(
        mixer_body,
        grid=(blocks,),
        in_specs=[
            pl.BlockSpec(memory_space=pltpu.SMEM),
            pl.BlockSpec(memory_space=pltpu.SMEM),
            pl.BlockSpec(memory_space=pltpu.SMEM),
            whole(HALO, 1024),
            pl.BlockSpec((BLOCK, 256), lambda i: (i, 0)),
            pl.BlockSpec((BLOCK, 256), lambda i: (i, 0)),
            pl.BlockSpec((2 * BLOCK, 128), lambda i: (i, 0)),
            pl.BlockSpec((2 * BLOCK, 128), lambda i: (i, 0)),
            pl.BlockSpec((4, BLOCK), lambda i: (0, i)),
            pl.BlockSpec((2, BLOCK), lambda i: (0, i)),
            whole(4, 256),
            whole(4, 256),
            whole(8, 128),
            whole(8, 128),
        ],
        out_specs=[
            pl.BlockSpec((BLOCK, 512), lambda i: (i, 0)),
            pl.BlockSpec((BLOCK, 256), lambda i: (i, 0)),
            pl.BlockSpec((8, BLOCK), lambda i: (0, i)),
            whole(BLOCK + 16, 256),
            whole(BLOCK + 16, 256),
        ],
        out_shape=[
            jax.ShapeDtypeStruct((length, 512), F32),
            jax.ShapeDtypeStruct((length, 256), BF16),
            jax.ShapeDtypeStruct((8, length), F32),
            jax.ShapeDtypeStruct((BLOCK + 16, 256), BF16),
            jax.ShapeDtypeStruct((BLOCK + 16, 256), BF16),
        ],
        scratch_shapes=[
            pltpu.VMEM((BLOCK + 8, 1024), F32),
            pltpu.VMEM((2, 2 * BLOCK, 128), F32),
            pltpu.VMEM((2, 8, BLOCK), F32),
            pltpu.VMEM((BLOCK, 512), F32),
            pltpu.VMEM((8, BLOCK), F32),
            pltpu.VMEM((8, 512), F32),
        ],
        name="mixer",
        cost_estimate=cost(11),
    )(core, small_decay, large_decay, halo, small, large, keys, queries, small_step, large_step, small_taps, large_taps, key_taps, query_taps)


def chip_body(core, keep, other, out):
    own, far = get_state(keep[...]), get_state(other[...])
    first = core[0] == 0
    early = [jnp.where(first, a, b) for a, b in zip(own, far)]
    late = [jnp.where(first, b, a) for a, b in zip(own, far)]
    put_state(out, *then(early, late))


def chip_state(core, keep, other):
    return pl.pallas_call(
        chip_body,
        in_specs=[pl.BlockSpec(memory_space=pltpu.SMEM)] + [pl.BlockSpec()] * 2,
        out_shape=jax.ShapeDtypeStruct(keep.shape, BF16),
        name="chip_state",
        cost_estimate=cost(1),
    )(core, keep, other)


def line_body(position, own, back1, back2, back3, total, inside, held):
    for back, ref in enumerate((own, back1, back2, back3)):
        held[(position[0] + 4 - back) % 4] = ref[...]
    inside[...] = jnp.zeros_like(inside)
    prefix = None
    for j in range(4):
        piece = get_state(held[j])
        if prefix is None:
            prefix = piece
        else:
            prefix = then(prefix, piece)

        @pl.when(position[0] == j + 1)
        def _():
            inside[0:BLOCK, :] = prefix[0]
            inside[BLOCK : BLOCK + 8, :] = prefix[1]

    put_state(total, *prefix)


def line_state(position, *pieces):
    shape = pieces[0].shape
    return pl.pallas_call(
        line_body,
        in_specs=[pl.BlockSpec(memory_space=pltpu.SMEM)] + [pl.BlockSpec()] * 4,
        out_shape=[
            jax.ShapeDtypeStruct(shape, BF16),
            jax.ShapeDtypeStruct((BLOCK + 8, shape[1]), F32),
        ],
        scratch_shapes=[pltpu.VMEM((4, *shape), BF16)],
        name="line_state",
        cost_estimate=cost(1),
    )(position, *pieces)


def entering_body(core, inside, back1, back2, back3, keep, other, mine, send):
    held = get_state(back3[...])
    held = then(held, get_state(back2[...]))
    held = then(held, get_state(back1[...]))
    held = then(held, (inside[0:BLOCK, :], inside[BLOCK : BLOCK + 8, :]))
    own, far = get_state(keep[...]), get_state(other[...])
    first = core[0] == 0
    early = [jnp.where(first, a, b) for a, b in zip(own, far)]
    second = then(held, early)
    mine[...] = jnp.where(first, held[0], second[0]).astype(BF16)
    send[...] = jnp.where(first, second[0], held[0]).astype(BF16)


def entering_state(core, inside, back1, back2, back3, keep, other):
    shape = jax.ShapeDtypeStruct((BLOCK, keep.shape[1]), BF16)
    return pl.pallas_call(
        entering_body,
        in_specs=[pl.BlockSpec(memory_space=pltpu.SMEM)] + [pl.BlockSpec()] * 6,
        out_shape=[shape, shape],
        name="entering",
        cost_estimate=cost(1),
    )(core, inside, back1, back2, back3, keep, other)


def gate_body(core, mix, query, cum, mine, other, small_gate, large_gate, small_gain, large_gain, out):
    first = core[0] == 0
    entering = [jnp.where(first, mine[...], other[...]), jnp.where(first, other[...], mine[...])]
    cum_t = cum[...].T
    cum_cols = column_pairs([jnp.broadcast_to(cum_t[:, h : h + 1], (BLOCK, BLOCK)) for h in range(6)])
    q = query[...]
    carried = jnp.concatenate(
        [
            jnp.dot(q[:, 128 * g : 128 * g + 128], entering[g], preferred_element_type=F32)
            for g in range(2)
        ],
        axis=1,
    )
    y = mix[...] + carried * jnp.exp(cum_cols)
    lane = lax.broadcasted_iota(jnp.int32, (BLOCK, 128), 1)
    low = lane < 64
    for n in range(4):
        gate = (small_gate if n < 2 else large_gate)[:, 128 * (n % 2) : 128 * (n % 2) + 128].astype(F32)
        gain = (small_gain if n < 2 else large_gain)[:, 128 * (n % 2) : 128 * (n % 2) + 128].astype(F32)
        gated = y[:, 128 * n : 128 * n + 128] * (gate * jax.nn.sigmoid(gate))
        square = gated * gated
        if n < 2:
            first = jnp.sum(jnp.where(low, square, 0.0), axis=1, keepdims=True)
            second = jnp.sum(jnp.where(low, 0.0, square), axis=1, keepdims=True)
            scale = jnp.where(low, lax.rsqrt(first / 64 + EPS), lax.rsqrt(second / 64 + EPS))
        else:
            scale = lax.rsqrt(jnp.sum(square, axis=1, keepdims=True) / 128 + EPS)
        out[:, 128 * n : 128 * n + 128] = (gated * scale * gain).astype(BF16)


def gated_heads(part, parts, core, mix, query, cum, mine, other, small_gate, large_gate, small_gain, large_gain):
    length = mix.shape[0]
    whole = lambda *shape: pl.BlockSpec(shape, lambda i: (0,) * len(shape))
    rows = lambda width: pl.BlockSpec((BLOCK, width), lambda i: (parts * i + part, 0))
    return pl.pallas_call(
        gate_body,
        grid=(length // BLOCK // parts,),
        in_specs=[
            pl.BlockSpec(memory_space=pltpu.SMEM),
            rows(512),
            rows(256),
            pl.BlockSpec((8, BLOCK), lambda i: (0, parts * i + part)),
            whole(BLOCK, 256),
            whole(BLOCK, 256),
            rows(256),
            rows(256),
            whole(1, 256),
            whole(1, 256),
        ],
        out_specs=pl.BlockSpec((BLOCK, 512), lambda i: (i, 0)),
        out_shape=jax.ShapeDtypeStruct((length // parts, 512), BF16),
        name="gated",
        cost_estimate=cost(4),
    )(core, mix, query, cum, mine, other, small_gate, large_gate, small_gain, large_gain)


SHARES = 4
WIDE_COLS = 256


def project_body(
    core, place, own, left, right, diag_low, diag_high,
    small_out, large_out, near_left, far_left, near_right, far_right, near_diag, far_diag,
    residual, mixer_gain, ffn_gain, normed_out, mixed_out, heads, acc,
):
    step = pl.program_id(0)
    width = own.shape[1] // 2
    rows = own.shape[0]

    @pl.when(step == 0)
    def _():
        heads[:, 0 : 2 * width] = own[...]
        first = core[0] == 0
        half = rows // 2
        parts = (
            (left, 0, rows, 1),
            (right, 0, rows, 2),
            (diag_low, 0, half, 3),
            (diag_high, half, rows, 3),
        )
        for ref, begin, end, n in parts:
            small, large = ref[:, 0:width], ref[:, width:]
            at = 2 * width * n
            heads[begin:end, at : at + width] = jnp.where(first, small, large)
            heads[begin:end, at + width : at + 2 * width] = jnp.where(first, large, small)

    weights = (small_out, large_out, near_left, far_left, near_right, far_right, near_diag, far_diag)
    out = jnp.dot(heads[:, 0:width], weights[0][...], preferred_element_type=F32)
    for n in range(1, 8):
        out = out + jnp.dot(heads[:, n * width : (n + 1) * width], weights[n][...], preferred_element_type=F32)
    acc[:, pl.ds(pl.multiple_of(step * WIDE_COLS, WIDE_COLS), WIDE_COLS)] = out

    @pl.when(step == pl.num_programs(0) - 1)
    def _():
        share = rows // SHARES
        few = 16
        for n, ahead in enumerate((0, 1, 3, 2)):
            at = (place[0] + ahead) % SHARES

            def one(k, _):
                mix = acc[pl.ds(pl.multiple_of(at * share + k * few, few), few), :]
                scale = lax.rsqrt(jnp.mean(mix * mix, axis=1, keepdims=True) + EPS)
                mixed = residual[at, 0, pl.ds(pl.multiple_of(k * few, few), few), :].astype(F32)
                mixed = mixed + mix * scale * mixer_gain[...].astype(F32)
                scale = lax.rsqrt(jnp.mean(mixed * mixed, axis=1, keepdims=True) + EPS)
                normed = mixed * scale * ffn_gain[...].astype(F32)
                normed_out[pl.ds(pl.multiple_of(n * share + k * few, few), few), :] = normed.astype(BF16)
                if n == 0:
                    mixed_out[pl.ds(pl.multiple_of(k * few, few), few), :] = mixed
                return 0

            lax.fori_loop(0, share // few, one, 0)


def project(part, parts, core, place, pieces, weights, residual, mixer_gain, ffn_gain):
    rows = pieces[0].shape[0]
    features = residual.shape[1]
    share = rows // SHARES
    whole = lambda a: pl.BlockSpec(a.shape, lambda i: (0, 0))
    return pl.pallas_call(
        project_body,
        grid=(features // WIDE_COLS,),
        in_specs=[pl.BlockSpec(memory_space=pltpu.SMEM)] * 2
        + [whole(p) for p in pieces]
        + [pl.BlockSpec((w.shape[0], WIDE_COLS), lambda i: (0, i)) for w in weights]
        + [
            pl.BlockSpec((SHARES, 1, share, features), lambda i: (0, part, 0, 0)),
            whole(mixer_gain),
            whole(ffn_gain),
        ],
        out_specs=[
            pl.BlockSpec((rows, features), lambda i: (0, 0)),
            pl.BlockSpec((share, features), lambda i: (0, 0)),
        ],
        out_shape=[
            jax.ShapeDtypeStruct((rows, features), BF16),
            jax.ShapeDtypeStruct((share, features), F32),
        ],
        scratch_shapes=[pltpu.VMEM((rows, features), BF16), pltpu.VMEM((rows, features), F32)],
        name="project",
        cost_estimate=cost(7),
    )(core, place, *pieces, *weights, residual.reshape(SHARES, parts, share, features), mixer_gain, ffn_gain)


def channel_body(x, proj, down, own, right, left, diag_low, diag_high, acc, hidden):
    step = pl.program_id(0)
    wide = hidden.shape[1]
    rows = x.shape[0]
    share = rows // SHARES

    @pl.when(step == 0)
    def _():
        acc[...] = jnp.dot(x[...], proj[...], preferred_element_type=F32)

    @pl.when(jnp.logical_and(step > 0, step < 4))
    def _():
        acc[...] += jnp.dot(x[...], proj[...], preferred_element_type=F32)

    @pl.when(step == 3)
    def _():
        few = 16

        def one(k, _):
            at = pl.ds(pl.multiple_of(k * few, few), few)
            gate = acc[at, 0:wide]
            hidden[at, :] = (gate * jax.nn.sigmoid(gate) * acc[at, wide:]).astype(BF16)
            return 0

        lax.fori_loop(0, rows // few, one, 0)

    @pl.when(step >= 4)
    def _():
        out = lax.dot_general(
            hidden[...], down[...], (((1,), (1,)), ((), ())), preferred_element_type=F32
        ).astype(BF16)
        own[...] = out[0:share]
        right[...] = out[share : 2 * share]
        left[...] = out[2 * share : 3 * share]
        diag_low[...] = out[3 * share : 3 * share + share // 2]
        diag_high[...] = out[3 * share + share // 2 :]


def channel(x, whole_proj):
    rows, features = x.shape
    wide = whole_proj.shape[1] // 3
    share = rows // SHARES
    deep = features // 4
    heights = (share, share, share, share // 2, share // 2)
    return pl.pallas_call(
        channel_body,
        grid=(8,),
        in_specs=[
            pl.BlockSpec((rows, deep), lambda i: (0, jnp.minimum(i, 3))),
            pl.BlockSpec((deep, 2 * wide), lambda i: (jnp.minimum(i, 3), 0)),
            pl.BlockSpec((deep, wide), lambda i: (jnp.maximum(i - 4, 0), 2)),
        ],
        out_specs=[pl.BlockSpec((h, deep), lambda i: (0, jnp.maximum(i - 4, 0))) for h in heights],
        out_shape=[jax.ShapeDtypeStruct((h, features), BF16) for h in heights],
        scratch_shapes=[pltpu.VMEM((rows, 2 * wide), F32), pltpu.VMEM((rows, wide), BF16)],
        name="channel",
        cost_estimate=cost(12),
    )(x, whole_proj, whole_proj)


def add_body(right, from_left, left, from_right, right_out, left_out):
    half = from_left.shape[0]
    right_out[half:, :] = right[half:, :]
    right_out[:half, :] = (right[:half, :].astype(F32) + from_left[...].astype(F32)).astype(BF16)
    left_out[:half, :] = left[:half, :]
    left_out[half:, :] = (left[half:, :].astype(F32) + from_right[...].astype(F32)).astype(BF16)


def add_passing(right, from_left, left, from_right):
    return pl.pallas_call(
        add_body,
        out_shape=[jax.ShapeDtypeStruct(right.shape, BF16), jax.ShapeDtypeStruct(left.shape, BF16)],
        name="add_passing",
        cost_estimate=cost(1),
    )(right, from_left, left, from_right)


def finish_body(*refs):
    *parts, gain, out = refs
    share = parts[0].shape[0]
    few = 16
    for n in range(len(parts) // 4):
        own, one_side, other_side, mixed = parts[4 * n : 4 * n + 4]

        def one(k, _):
            at = pl.ds(pl.multiple_of(k * few, few), few)
            ffn = own[at, :].astype(F32) + one_side[at, :].astype(F32) + other_side[at, :].astype(F32)
            scale = 0.5 * lax.rsqrt(jnp.mean(ffn * ffn, axis=1, keepdims=True) + EPS)
            done = mixed[at, :] + ffn * scale * gain[...].astype(F32)
            out[pl.ds(pl.multiple_of(n * share + k * few, few), few), :] = done.astype(BF16)
            return 0

        lax.fori_loop(0, share // few, one, 0)


def finish(parts, gain):
    share, features = parts[0][0].shape
    flat = [a for part in parts for a in part]
    return pl.pallas_call(
        finish_body,
        out_shape=jax.ShapeDtypeStruct((len(parts) * share, features), BF16),
        name="finish",
        cost_estimate=cost(3),
    )(*flat, gain)


SP = ("sp_0", "sp_1", "sp_2")
SP_TP = ("sp_0", "sp_1", "sp_2", "tp")


PARTS = 2


def turned(axis, distance):
    size = lax.axis_size(axis)
    return [(i, (i + distance) % size) for i in range(size)]


def onward(axis, distance):
    size = lax.axis_size(axis)
    return [(i, i + distance) for i in range(size - distance)]


def round_line(array, axis):
    half = array.shape[0] // 2
    left = lax.ppermute(array, axis, turned(axis, 1))
    right = lax.ppermute(array, axis, turned(axis, -1))
    low = lax.ppermute(left[:half], axis, turned(axis, 1))
    high = lax.ppermute(right[half:], axis, turned(axis, -1))
    return [array, left, right, low, high]


def scalar(value):
    return value.astype(jnp.int32).reshape(1)


def local(
    residual,
    small_heads,
    large_heads,
    state_keys,
    state_queries,
    small_gate,
    large_gate,
    small_step,
    large_step,
    small_taps,
    large_taps,
    key_taps,
    query_taps,
    small_decay,
    large_decay,
    small_gain,
    large_gain,
    small_out,
    large_out,
    mixer_gain,
    ffn_in_gain,
    gate_proj,
    up_proj,
    down_proj,
    ffn_out_gain,
):
    length = residual.shape[0]
    wide = gate_proj.shape[1]
    whole_proj = lax.all_gather(
        jnp.concatenate([gate_proj, up_proj, down_proj], axis=1), SP, axis=0, tiled=True
    )
    keys = state_keys.reshape(2 * length, 128)
    queries = state_queries.reshape(2 * length, 128)
    devices = range(lax.axis_size(SP))
    halo = lax.ppermute(
        pack_halo(small_heads, large_heads, keys, queries), SP, [(i, i + 1) for i in devices[:-1]]
    )
    core = scalar(lax.axis_index("sp_2"))
    place = scalar(lax.axis_index("tp"))
    mix, query_conv, cum, keep, send = mixer(
        core,
        halo,
        small_heads,
        large_heads,
        keys,
        queries,
        small_step.T,
        large_step.T,
        small_taps,
        large_taps,
        key_taps.reshape(8, 128),
        query_taps.reshape(8, 128),
        small_decay,
        large_decay,
    )
    near = jnp.where(core == 0, small_out, large_out)
    near_out = [lax.ppermute(near, "tp", turned("tp", d)) for d in (1, -1, 2)]
    far_out = [lax.ppermute(a, "sp_2", turned("sp_2", 1)) for a in near_out]
    out_weights = [small_out, large_out]
    for a, b in zip(near_out, far_out):
        out_weights += [a, b]

    other = lax.ppermute(send, "sp_2", turned("sp_2", 1))
    chip = chip_state(core, keep, other)
    line, inside = line_state(
        scalar(lax.axis_index("sp_1")),
        chip,
        *[lax.ppermute(chip, "sp_1", turned("sp_1", d)) for d in (1, 2, 3)],
    )
    mine, send = entering_state(
        core, inside, *[lax.ppermute(line, "sp_0", onward("sp_0", d)) for d in (1, 2, 3)], keep, other
    )
    theirs = lax.ppermute(send, "sp_2", turned("sp_2", 1))

    parts = []
    for part in range(PARTS):
        normed = gated_heads(
            part,
            PARTS,
            core,
            mix,
            query_conv,
            cum,
            mine,
            theirs,
            small_gate,
            large_gate,
            small_gain.reshape(1, -1),
            large_gain.reshape(1, -1),
        )
        pieces = round_line(normed, "tp")
        normed_in, mixed = project(
            part,
            PARTS,
            core,
            place,
            pieces,
            out_weights,
            residual,
            mixer_gain.reshape(1, -1),
            ffn_in_gain.reshape(1, -1),
        )
        own, right, left, low, high = channel(normed_in, whole_proj)
        low = lax.ppermute(low, "tp", turned("tp", 1))
        high = lax.ppermute(high, "tp", turned("tp", -1))
        right, left = add_passing(right, low, left, high)
        parts.append(
            (
                own,
                lax.ppermute(right, "tp", turned("tp", 1)),
                lax.ppermute(left, "tp", turned("tp", -1)),
                mixed,
            )
        )
    return finish(parts, ffn_out_gain.reshape(1, -1))


def solution(mesh):
    torus = Mesh(mesh.devices.reshape(4, 4, 2, mesh.shape["tp"]), ("sp_0", "sp_1", "sp_2", "tp"))
    in_specs = (
        P(SP, None),
        P(SP, "tp"),
        P(SP, "tp"),
        P(SP, "tp", None),
        P(SP, "tp", None),
        P(SP, "tp"),
        P(SP, "tp"),
        P(SP, "tp"),
        P(SP, "tp"),
        P(None, "tp"),
        P(None, "tp"),
        P(None, "tp", None),
        P(None, "tp", None),
        P("tp"),
        P("tp"),
        P("tp"),
        P("tp"),
        P("tp", None),
        P("tp", None),
        P(),
        P(),
        P(SP, "tp"),
        P(SP, "tp"),
        P(SP, "tp"),
        P(),
    )
    out_specs = P(SP_TP, None)
    return jax.shard_map(local, mesh=torus, in_specs=in_specs, out_specs=out_specs, check_vma=False)
```
